512 devices in a mesh: sp: 64 (over z, y), tp: 8 (over x, core).
Axes of the slice: x: 4, y: 4, z: 16, core: 2. Of those that a mesh axis runs over, the one named last changes fastest.
Arguments:
- resid: bfloat16 [12288, 2048], P('sp'), may hold values from -6 to 6
- queries: bfloat16 [12288, 1024], P('sp', 'tp'), may hold values from -6.5 to 6.5
- keys: bfloat16 [12288, 1024], P('sp', 'tp'), may hold values from -6.5 to 6.5
- values: bfloat16 [12288, 1024], P('sp', 'tp'), may hold values from -6 to 6
- lambdas: float32 [8], P('tp'), may hold values from 0.3 to 0.8
- head_gain: float32 [128], replicated, may hold values from 0.1 to 1.9
- out_weight: bfloat16 [1024, 2048], P('tp'), may hold values from -0.1875 to 0.1875
- norm_gain: float32 [2048], replicated, may hold values from 0.1 to 1.9
- gate_weight: bfloat16 [2048, 5632], P('sp', 'tp'), may hold values from -0.125 to 0.125
- up_weight: bfloat16 [2048, 5632], P('sp', 'tp'), may hold values from -0.125 to 0.125
- down_weight: bfloat16 [5632, 2048], P('tp', 'sp'), may hold values from -0.078125 to 0.078125
Outputs:
- result: bfloat16 [12288, 2048], P('sp')
The draws below stay inside these ranges and needn't reach their ends.
All inputs are finite; a program needn't handle non-finite values.
Results may differ from the reference program's by a relative error of at most 0.014.
Values may be sent and summed in bfloat16 or wider, within the bound.
A program may use at most 128 MiB of HBM per device.

```python
import jax
import jax.numpy as jnp
from jax import lax

D = 2048
HEADS = 8
QK = 64
VD = 128
FF = 5632
TOK_DEV = 192
TOKENS = 12288
N_TP = 8


def shared_field(key, salt, planted_row, period):
    width = HEADS * 2 * QK
    field = jnp.clip(jax.random.normal(jax.random.fold_in(key, salt), (TOKENS, width), jnp.float32) * 1.3, -6.5, 6.5)
    return field


def draw_queries(key, part):
    return shared_field(key, 11, 5, 97).astype(jnp.bfloat16)


def draw_keys(key, part):
    return shared_field(key, 23, 3, 89).astype(jnp.bfloat16)


def level_of(own_key, shape, cuts, low, high):
    factor_of, own = 1.0, jax.random.fold_in(own_key, 6)
    for position, blocks in cuts:
        steps = jnp.exp(jax.random.uniform(jax.random.fold_in(own, position), (blocks,), jnp.float32, low / len(cuts), high / len(cuts)))
        factor_of = factor_of * jnp.repeat(steps, shape[position] // blocks).reshape([-1 if axis == position else 1 for axis in range(len(shape))])
    return factor_of


def normal_values(stream_key, extent, scale, bound, cuts=(), kind=jnp.bfloat16):
    gain = level_of(stream_key, extent, cuts, -0.22, 0.18) if cuts else 1.0
    array = jax.random.normal(stream_key, extent, jnp.float32) * scale * gain
    return jnp.minimum(jnp.maximum(array, -bound), bound).astype(kind)


def setup_inputs(seed: int = 0) -> dict:
    splits = jax.random.split(jax.random.key(seed), 12)
    resid = normal_values(splits[0], (TOKENS, D), 1.0, 6.0, ((0, 64),))
    queries = draw_queries(jax.random.fold_in(splits[11], 71), 0)
    keys = draw_keys(jax.random.fold_in(splits[11], 71), 0)
    values = normal_values(splits[3], (TOKENS, HEADS * VD), 1.0, 6.0, ((0, 64), (1, 8)))
    lambdas = jnp.clip(0.3 + 0.5 * jax.random.uniform(splits[4], (HEADS,), jnp.float32) ** level_of(splits[4], (HEADS,), ((0, 8),), -0.2, 0.2), 0.3, 0.8)
    head_gain = jnp.clip(1.0 + 0.18 * jax.random.normal(splits[5], (VD,), jnp.float32), 0.1, 1.9)
    out_weight = normal_values(splits[6], (HEADS * VD, D), (HEADS * VD) ** -0.5, 0.1875, ((0, 8),))
    norm_gain = jnp.clip(1.0 + 0.18 * jax.random.normal(splits[7], (D,), jnp.float32), 0.1, 1.9)
    gate_weight = normal_values(splits[8], (D, FF), D ** -0.5, 0.125, ((0, 64), (1, 8)))
    up_weight = normal_values(splits[9], (D, FF), D ** -0.5, 0.125, ((0, 64), (1, 8)))
    down_weight = normal_values(splits[10], (FF, D), FF ** -0.5, 0.078125, ((0, 8), (1, 64)))
    return dict(resid=resid, queries=queries, keys=keys, values=values, lambdas=lambdas, head_gain=head_gain, out_weight=out_weight, norm_gain=norm_gain, gate_weight=gate_weight, up_weight=up_weight, down_weight=down_weight)


def reference(resid, queries, keys, values, lambdas, head_gain, out_weight, norm_gain, gate_weight, up_weight, down_weight):
    tok_total = resid.shape[0]
    head_count = lambdas.shape[0]
    query_all = queries.reshape(tok_total, head_count, 2, QK).astype(jnp.float32)
    key_all = keys.reshape(tok_total, head_count, 2, QK).astype(jnp.float32)
    value_all = values.reshape(tok_total, head_count, VD).astype(jnp.float32)
    score_scale = QK ** (-0.5)
    key_pos = jnp.arange(tok_total, dtype=jnp.int32)

    def one_block(block_index):
        block_start = (block_index * TOK_DEV).astype(jnp.int32)
        query_block = lax.dynamic_slice_in_dim(query_all, block_start, TOK_DEV, 0)
        scores = jnp.einsum('qhcd,khcd->chqk', query_block, key_all) * score_scale
        query_pos = block_start + jnp.arange(TOK_DEV, dtype=jnp.int32)
        causal_mask = key_pos[None, :] <= query_pos[:, None]
        scores = jnp.where(causal_mask, scores, -1e+30)
        row_max = lax.optimization_barrier(jnp.max(scores, axis=-1, keepdims=True))
        expo = jnp.where(causal_mask, jnp.exp(scores - row_max), 0.0)
        row_sum = lax.optimization_barrier(jnp.sum(expo, axis=-1))
        rounded = lax.optimization_barrier(expo.astype(jnp.bfloat16)).astype(jnp.float32)
        numer = jnp.einsum('chqk,khd->chqd', rounded, value_all)
        ratio = numer / row_sum[..., None]
        mixed_heads = ratio[0] - lambdas[:, None, None] * ratio[1]
        normed_heads = mixed_heads * lax.rsqrt(lax.optimization_barrier(jnp.mean(mixed_heads * mixed_heads, axis=-1, keepdims=True)) + 1e-05) * head_gain
        return jnp.transpose(normed_heads.astype(jnp.bfloat16), (1, 0, 2))
    head_out = lax.map(one_block, jnp.arange(tok_total // TOK_DEV, dtype=jnp.int32)).reshape(tok_total, head_count * VD)
    group_cols = head_count // N_TP * VD
    branch = jnp.zeros((tok_total, resid.shape[1]), jnp.float32)
    for group in range(N_TP):
        partial_sum = jnp.dot(head_out[:, group * group_cols:(group + 1) * group_cols], out_weight[group * group_cols:(group + 1) * group_cols], preferred_element_type=jnp.float32)
        branch = branch + partial_sum.astype(jnp.bfloat16).astype(jnp.float32)
    first = resid.astype(jnp.float32) + branch
    normed = (first * lax.rsqrt(lax.optimization_barrier(jnp.mean(first * first, axis=-1, keepdims=True)) + 1e-06) * norm_gain).astype(jnp.bfloat16)
    hidden_group = FF // N_TP
    mixer = jnp.zeros_like(first)
    for group in range(N_TP):
        cols = slice(group * hidden_group, (group + 1) * hidden_group)
        gate_act = jnp.dot(normed, gate_weight[:, cols], preferred_element_type=jnp.float32)
        up_act = jnp.dot(normed, up_weight[:, cols], preferred_element_type=jnp.float32)
        hidden = (jax.nn.silu(gate_act) * up_act).astype(jnp.bfloat16)
        partial_sum = jnp.dot(hidden, down_weight[cols, :], preferred_element_type=jnp.float32)
        mixer = mixer + partial_sum.astype(jnp.bfloat16).astype(jnp.float32)
    return (first + 0.5 * mixer).astype(jnp.bfloat16)
```

```python
import functools
import math

import jax
import jax.numpy as jnp
from jax import lax
from jax.experimental import pallas as pl
from jax.experimental.pallas import tpu as pltpu
from jax.sharding import Mesh
from jax.sharding import PartitionSpec as P

QK = 64
VD = 128
LANES = 128
NC = 2
SP = ("z", "y")
TP = ("x", "c")
MESH = pl.DeviceIdType.MESH
SEMS = 200
SCALE2 = QK ** (-0.5) * math.log2(math.e)
NEG = -1e30


def dot_nt(a, b):
    return lax.dot_general(a, b, (((1,), (1,)), ((), ())), preferred_element_type=jnp.float32)


def dot_nn(a, b):
    return jnp.dot(a, b, preferred_element_type=jnp.float32)


def kernel(
    nz,
    ny,
    nx,
    lam_ref,
    q_ref,
    k_ref,
    v_ref,
    hg_ref,
    ow_ref,
    ng_ref,
    resid_ref,
    gu_ref,
    dn_ref,
    out_ref,
    kb,
    vb,
    qb,
    qm,
    acc,
    mx,
    ls,
    rb,
    mb,
    gu,
    dstage,
    dn,
    pf,
    pown,
    pair,
    sx,
    rx,
    first,
    ss,
    ss_in,
    nall,
    fb,
    fown,
    pair2,
    gs,
    ra,
    rbx,
    sa,
    sb,
    ra2,
    rb2,
    send_sem,
    recv_sem,
):
    z, y, x, c = (lax.axis_index(a) for a in ("z", "y", "x", "c"))
    R = q_ref.shape[0]
    Rx = R // nx
    Dc = resid_ref.shape[1] // NC
    D = NC * Dc
    H = Dc // 2
    h = dn_ref.shape[1]
    GR = ny * gu_ref.shape[1]
    RS = gu_ref.shape[1]
    bf = jnp.bfloat16
    f32 = jnp.float32

    def at(axis, d):
        me, n = {"z": (z, nz), "y": (y, ny), "x": (x, nx)}[axis]
        return lax.rem(me + (d + n), n)

    def mult(v, m):
        return pl.multiple_of(v, m)

    up, down = {"z": at("z", 1)}, {"z": at("z", -1)}
    partner = {"c": 1 - c}
    peers = [up, down, partner]
    peers += [{"y": at("y", d)} for d in range(1, ny)]
    peers += [{"x": at("x", d)} for d in range(1, nx)]
    barrier = pltpu.get_barrier_semaphore()
    for p in peers:
        pl.semaphore_signal(barrier, inc=1, device_id=p, device_id_type=MESH)
    pl.semaphore_wait(barrier, len(peers))

    started = []

    def send(src, dst, to):
        k = len(started)
        copy = pltpu.make_async_remote_copy(
            src_ref=src,
            dst_ref=dst,
            send_sem=send_sem.at[k],
            recv_sem=recv_sem.at[k],
            device_id=to,
            device_id_type=MESH,
        )
        copy.start()
        started.append(copy)
        return copy

    U, W = nz // 2, (nz - 1) // 2
    ku, vu, kd, vd = ({} for _ in range(4))
    ku[1] = send(k_ref, kb.at[z], up)
    kd[1] = send(k_ref, kb.at[z], down)
    qs = [send(q_ref, qb.at[y], {"y": at("y", d)}) for d in range(1, ny)]
    vu[1] = send(v_ref, vb.at[z], up)
    vd[1] = send(v_ref, vb.at[z], down)

    def gu_slot(zz):
        return gu.at[pl.ds(mult(zz * GR, GR), GR)]

    def dn_slot(zz):
        return dn.at[pl.ds(0, h), pl.ds(mult(zz * LANES, LANES), LANES)]

    ws = []
    for d in range(1, ny):
        to = at("y", d)
        row = mult(z * GR + y * RS, RS)
        ws.append(send(gu_ref.at[to], gu.at[pl.ds(row, RS)], {"y": to}))
        ws.append(send(dn_ref.at[to], dstage.at[y], {"y": to}))

    qb[y] = q_ref[...]
    gu[pl.ds(mult(z * GR + y * RS, RS), RS), :] = gu_ref[y]
    dn[pl.ds(h, dn.shape[0] - h), :] = jnp.zeros((dn.shape[0] - h, D), bf)
    for a in qs:
        a.wait_recv()
    lane = lax.broadcasted_iota(jnp.int32, (R, LANES), 1)
    for yy in range(ny):
        block = qb[yy]
        zero = jnp.zeros_like(block)
        qm[yy * R : (yy + 1) * R, :] = jnp.where(lane < QK, block, zero)
        qm[(ny + yy) * R : (ny + yy + 1) * R, :] = jnp.where(lane < QK, zero, block)
    acc[...] = jnp.zeros_like(acc)
    ls[...] = jnp.zeros_like(ls)
    mx[...] = jnp.full(mx.shape, NEG, f32)

    def attend(load, masked):
        def body(i, carry):
            rows = pl.ds(mult(i * R, R), R)
            keys, vals = load()
            s = dot_nt(qm[rows, :], keys)
            if masked:
                kpos = y * R + lax.broadcasted_iota(jnp.int32, s.shape, 1)
                qpos = lax.rem(i, ny) * R + lax.broadcasted_iota(jnp.int32, s.shape, 0)
                keep = kpos <= qpos
                s = jnp.where(keep, s, NEG)
            old = mx[rows, :]
            new = jnp.maximum(old, jnp.max(s, axis=-1, keepdims=True))
            e = jnp.exp2((s - new[:, :1]) * SCALE2)
            if masked:
                e = jnp.where(keep, e, 0.0)
            factor = jnp.exp2((old - new) * SCALE2)
            mx[rows, :] = new
            ls[rows, :] = ls[rows, :] * factor + jnp.sum(e, axis=-1, keepdims=True)
            acc[rows, :] = acc[rows, :] * factor + dot_nn(e.astype(bf), vals)
            return carry

        lax.fori_loop(0, 2 * ny, body, 0)

    attend(lambda: (k_ref[...], v_ref[...]), True)

    for a in ws:
        a.wait_recv()
    dn_mine = dn_ref[y]
    for d in range(1, ny):
        dn_mine = dn_mine + dstage[at("y", -d)]
    dn[pl.ds(0, h), pl.ds(mult(z * LANES, LANES), LANES)] = dn_mine

    for s in range(1, U + 1):
        zu, zd = at("z", -s), at("z", s)
        ku[s].wait_recv()
        if s < U:
            ku[s + 1] = send(kb.at[zu], kb.at[zu], up)
        if s <= W:
            kd[s].wait_recv()
            if s < W:
                kd[s + 1] = send(kb.at[zd], kb.at[zd], down)
        vu[s].wait_recv()
        if s < U:
            vu[s + 1] = send(vb.at[zu], vb.at[zu], up)
        if s <= W:
            vd[s].wait_recv()
            if s < W:
                vd[s + 1] = send(vb.at[zd], vb.at[zd], down)

        def one(zu=zu):
            attend(lambda: (kb[zu], vb[zu]), False)

        def two(zu=zu, zd=zd):
            attend(
                lambda: (
                    jnp.concatenate([kb[zu], kb[zd]], axis=0),
                    jnp.concatenate([vb[zu], vb[zd]], axis=0),
                ),
                False,
            )

        if s <= W:
            pl.when(z >= nz - s)(two)
            pl.when((z >= s) & (z < nz - s))(one)
        else:
            pl.when(z >= s)(one)

    gu_u, dn_u, gu_d, dn_d = ({} for _ in range(4))

    def weight_step(s):
        if s > U:
            return
        zu, zd = at("z", -s), at("z", s)
        if s > 0:
            gu_u[s].wait_recv()
        if s < U:
            gu_u[s + 1] = send(gu_slot(zu), gu_slot(zu), up)
        if 0 < s <= W:
            gu_d[s].wait_recv()
        if s < W:
            gu_d[s + 1] = send(gu_slot(zd), gu_slot(zd), down)
        if s > 0:
            dn_u[s].wait_recv()
        if s < U:
            dn_u[s + 1] = send(dn_slot(zu), dn_slot(zu), up)
        if 0 < s <= W:
            dn_d[s].wait_recv()
        if s < W:
            dn_d[s + 1] = send(dn_slot(zd), dn_slot(zd), down)

    weight_step(0)

    def partial(yy):
        tile = jnp.zeros((R, LANES), f32)
        for m in range(2):
            rows = pl.ds(mult((m * ny + yy) * R, R), R)
            total = ls[rows, :]
            some = total > 0.0
            safe = jnp.where(some, total, 1.0)
            rb[yy, :, m * VD : (m + 1) * VD] = (acc[rows, :] / safe).astype(bf)
            lse = jnp.where(some, mx[rows, :] * SCALE2 + jnp.log2(safe), NEG)
            high = lse.astype(bf).astype(f32)
            rest = lse - high
            middle = rest.astype(bf).astype(f32)
            low = rest - middle
            for j, piece in enumerate((high, middle, low)):
                tile = jnp.where(lane == 3 * m + j, piece, tile)
        rb[yy, :, 2 * VD :] = tile.astype(bf)

    ms = []
    for d in range(1, ny):
        to = at("y", d)
        partial(to)
        ms.append(send(rb.at[to], mb.at[y], {"y": to}))
    partial(y)
    weight_step(1)
    for a in ms:
        a.wait_recv()
    parts = [rb.at[y]] + [mb.at[at("y", -d)] for d in range(1, ny)]
    ratios = []
    for m in range(2):
        lses = []
        for part in parts:
            t = part[:, 2 * VD :].astype(f32)
            mine = (lane >= 3 * m) & (lane < 3 * m + 3)
            lses.append(jnp.sum(jnp.where(mine, t, 0.0), axis=-1, keepdims=True))
        top = functools.reduce(jnp.maximum, lses)
        weights = [jnp.exp2(v - top) for v in lses]
        total = functools.reduce(jnp.add, weights)
        numer = functools.reduce(
            jnp.add,
            [w * part[:, m * VD : (m + 1) * VD].astype(f32) for w, part in zip(weights, parts)],
        )
        ratios.append(numer / total)
    mixed = ratios[0] - lam_ref[0] * ratios[1]
    head = (
        mixed
        * lax.rsqrt(jnp.mean(mixed * mixed, axis=-1, keepdims=True) + 1e-05)
        * hg_ref[...]
    ).astype(bf)

    other_cols = pl.ds(mult((1 - c) * Dc, Dc), Dc)
    own_cols = pl.ds(mult(c * Dc, Dc), Dc)
    pf[...] = dot_nn(head, ow_ref[:, other_cols]).astype(bf)
    pc = send(pf, pair, partner)
    pown[...] = dot_nn(head, ow_ref[:, own_cols])
    weight_step(2)
    pc.wait_recv()
    xs = []
    for d in range(1, nx):
        to = at("x", d)
        rows = pl.ds(mult(to * Rx, Rx), Rx)
        sx[rows, :] = (pown[rows, :] + pair[rows, :].astype(f32)).astype(bf)
        xs.append(send(sx.at[rows], rx.at[x], {"x": to}))
    my_rows = pl.ds(mult(x * Rx, Rx), Rx)
    total = pown[my_rows, :] + pair[my_rows, :].astype(f32)
    total = total + resid_ref[my_rows, own_cols].astype(f32)
    for a in xs:
        a.wait_recv()
    for d in range(1, nx):
        total = total + rx[at("x", -d)].astype(f32)
    first[...] = total
    ss[...] = jnp.broadcast_to(jnp.sum(total * total, axis=-1, keepdims=True), ss.shape)
    sc = send(ss, ss_in, partner)
    weight_step(3)
    sc.wait_recv()
    mean = (ss[...] + ss_in[...])[:, :1] * (1.0 / D)
    normed = (first[...] * lax.rsqrt(mean + 1e-06) * ng_ref[c]).astype(bf)

    def block(yy, xx, half):
        row = mult(yy * R + xx * Rx, Rx)
        return nall.at[c, pl.ds(row, Rx), pl.ds(half * H, H)]

    nall[c, pl.ds(mult(y * R + x * Rx, Rx), Rx), :] = normed

    xa, yb, far_a, far_b, local = {}, {}, [], [], []
    ring = {"x": nx, "y": ny}

    def pass_on(ref, axis):
        return [send(ref, ref, {axis: at(axis, d)}) for d in range(1, ring[axis])]

    first_a = pass_on(block(y, x, 0), "x")
    first_b = pass_on(block(y, x, 1), "y")
    for half, axis, far in ((0, "y", far_a), (1, "x", far_b)):
        far.append(pass_on(block(y, x, half), axis))
        local.append(send(block(y, x, half), block(y, x, half), partner))
    weight_step(4)
    for e in range(1, max(nx, ny)):
        if e < nx:
            first_a[e - 1].wait_recv()
            ref = block(y, at("x", -e), 0)
            far_a.append(pass_on(ref, "y"))
            local.append(send(ref, ref, partner))
        if e < ny:
            first_b[e - 1].wait_recv()
            ref = block(at("y", -e), x, 1)
            far_b.append(pass_on(ref, "x"))
            local.append(send(ref, ref, partner))
    weight_step(5)
    for e in range(max(nx, ny)):
        if e < nx:
            for d in range(1, ny):
                far_a[e][d - 1].wait_recv()
                ref = block(at("y", -d), at("x", -e), 0)
                local.append(send(ref, ref, partner))
        if e < ny:
            for d in range(1, nx):
                far_b[e][d - 1].wait_recv()
                ref = block(at("y", -e), at("x", -d), 1)
                local.append(send(ref, ref, partner))
    for s in range(6, U + 1):
        weight_step(s)
    for a in local:
        a.wait_recv()

    chunk_lane = lax.broadcasted_iota(jnp.int32, (R, LANES), 1)
    p2 = []
    order = [at("y", d) for d in range(1, ny)] + [y]
    for yy in order:
        rows = pl.ds(mult(yy * R, R), R)
        t = dot_nn(nall[0, rows, :], gu[:Dc, :]) + dot_nn(nall[1, rows, :], gu[Dc:, :])
        t0, t1, t2 = (t[:, j * LANES : (j + 1) * LANES] for j in range(3))
        h0 = t0 / (1.0 + jnp.exp(-t0)) * t2
        h1 = t1 / (1.0 + jnp.exp(-t1)) * pltpu.roll(t1, 64, 1)
        h1 = jnp.where(chunk_lane < h - LANES, h1, 0.0)
        hidden = jnp.concatenate([h0, h1], axis=1).astype(bf)
        fb[rows, :] = dot_nn(hidden, dn[:, other_cols]).astype(bf)
        p2.append(send(fb.at[rows], pair2.at[rows], partner))
        fown[rows, :] = dot_nn(hidden, dn[:, own_cols])

    sa1, sb1 = [], []
    left, right = slice(0, H), slice(H, Dc)
    for j, yy in enumerate(order):
        rows = pl.ds(mult(yy * R, R), R)
        p2[j].wait_recv()
        both = fown[rows, :] + pair2[rows, :].astype(f32)
        fown[rows, :] = both
        gs[rows, :] = both.astype(bf)
        if j < ny - 1:
            sa1.append(send(gs.at[rows, left], ra.at[y], {"y": yy}))
        for d in range(1, nx):
            to = at("x", d)
            piece = pl.ds(mult(yy * R + to * Rx, Rx), Rx)
            sb1.append(send(gs.at[piece, right], rbx.at[x, yy], {"x": to}))
    for a in sa1:
        a.wait_recv()
    rows = pl.ds(mult(y * R, R), R)
    half_a = fown[rows, left]
    for d in range(1, ny):
        half_a = half_a + ra[at("y", -d)].astype(f32)
    fown[rows, left] = half_a
    sa[...] = half_a.astype(bf)
    sa2 = []
    for d in range(1, nx):
        to = at("x", d)
        sa2.append(send(sa.at[pl.ds(mult(to * Rx, Rx), Rx)], ra2.at[x], {"x": to}))
    for a in sb1:
        a.wait_recv()
    sb2 = []
    for yy in order:
        piece = pl.ds(mult(yy * R + x * Rx, Rx), Rx)
        half_b = fown[piece, right]
        for d in range(1, nx):
            half_b = half_b + rbx[at("x", -d), yy].astype(f32)
        if len(sb2) < ny - 1:
            sb[yy] = half_b.astype(bf)
            sb2.append(send(sb.at[yy], rb2.at[y], {"y": yy}))
    mine = pl.ds(mult(y * R + x * Rx, Rx), Rx)
    mix_a = fown[mine, left]
    for a in sa2:
        a.wait_recv()
    for d in range(1, nx):
        mix_a = mix_a + ra2[at("x", -d)].astype(f32)
    for a in sb2:
        a.wait_recv()
    mix_b = half_b
    for d in range(1, ny):
        mix_b = mix_b + rb2[at("y", -d)].astype(f32)
    mixer = jnp.concatenate([mix_a, mix_b], axis=1)
    out_ref[my_rows, own_cols] = (first[...] + 0.5 * mixer).astype(bf)

    def tile(xx):
        return out_ref.at[pl.ds(mult(xx * Rx, Rx), Rx), own_cols]

    fx = pass_on(tile(x), "x")
    last = [send(tile(x), tile(x), partner)]
    for d in range(1, nx):
        fx[d - 1].wait_recv()
        ref = tile(at("x", -d))
        last.append(send(ref, ref, partner))
    for a in last:
        a.wait_recv()
    for a in started:
        a.wait_send()


def local(
    nz,
    ny,
    nx,
    resid,
    queries,
    keys,
    values,
    lambdas,
    head_gain,
    out_weight,
    norm_gain,
    gate_weight,
    up_weight,
    down_weight,
):
    R, D = resid.shape
    RS, F = gate_weight.shape
    h = F // ny
    CS = down_weight.shape[1]
    Rx, Dc = R // nx, D // NC
    H = Dc // 2
    bf, f32 = jnp.bfloat16, jnp.float32
    assert LANES < h <= LANES + 64 and CS * ny == LANES and queries.shape[1] == LANES

    def cut(w):
        return jnp.moveaxis(w.reshape(RS, ny, h), 1, 0)

    g, u = cut(gate_weight), cut(up_weight)
    fill = jnp.zeros((ny, RS, 64 - (h - LANES)), bf)
    gu = jnp.concatenate(
        [g[..., :LANES], g[..., LANES:], fill, u[..., LANES:], fill, u[..., :LANES]], axis=-1
    )
    place = lax.broadcasted_iota(jnp.int32, (1, 1, LANES), 2) // CS == lax.axis_index("y")
    dn = jnp.where(place, jnp.tile(down_weight.reshape(ny, h, CS), (1, 1, ny)), 0)

    vm = pl.BlockSpec(memory_space=pltpu.VMEM)
    scratch = [
        ((nz, R, LANES), bf),
        ((nz, R, LANES), bf),
        ((ny, R, LANES), bf),
        ((2 * ny * R, LANES), bf),
        ((2 * ny * R, LANES), f32),
        ((2 * ny * R, LANES), f32),
        ((2 * ny * R, LANES), f32),
        ((ny, R, 3 * LANES), bf),
        ((ny, R, 3 * LANES), bf),
        ((D, 3 * LANES), bf),
        ((ny, h, LANES), bf),
        ((2 * LANES, D), bf),
        ((R, Dc), bf),
        ((R, Dc), f32),
        ((R, Dc), bf),
        ((R, Dc), bf),
        ((nx, Rx, Dc), bf),
        ((Rx, Dc), f32),
        ((Rx, LANES), f32),
        ((Rx, LANES), f32),
        ((NC, ny * R, Dc), bf),
        ((ny * R, Dc), bf),
        ((ny * R, Dc), f32),
        ((ny * R, Dc), bf),
        ((ny * R, Dc), bf),
        ((ny, R, H), bf),
        ((nx, ny, Rx, H), bf),
        ((R, H), bf),
        ((ny, Rx, H), bf),
        ((nx, Rx, H), bf),
        ((ny, Rx, H), bf),
    ]
    return pl.pallas_call(
        functools.partial(kernel, nz, ny, nx),
        out_shape=jax.ShapeDtypeStruct((R, D), bf),
        in_specs=[pl.BlockSpec(memory_space=pltpu.SMEM)] + [vm] * 9,
        out_specs=vm,
        scratch_shapes=[pltpu.VMEM(*s) for s in scratch]
        + [pltpu.SemaphoreType.DMA((SEMS,)), pltpu.SemaphoreType.DMA((SEMS,))],
        compiler_params=pltpu.CompilerParams(
            collective_id=0, has_side_effects=True, vmem_limit_bytes=56 * 1024 * 1024
        ),
    )(
        lambdas,
        queries,
        keys,
        values,
        head_gain.reshape(1, VD),
        out_weight,
        norm_gain.reshape(NC, 1, Dc),
        resid,
        gu,
        dn,
    )


def solution(mesh):
    tp = mesh.shape["tp"]
    sp = mesh.shape["sp"]
    ny = 4 if sp == 64 else 2
    nz, nx = sp // ny, tp // NC
    finer = Mesh(mesh.devices.reshape(nz, ny, nx, NC), ("z", "y", "x", "c"))
    return jax.shard_map(
        functools.partial(local, nz, ny, nx),
        mesh=finer,
        in_specs=(
            P(SP, None),
            P(SP, TP),
            P(SP, TP),
            P(SP, TP),
            P(TP),
            P(),
            P(TP, None),
            P(),
            P(SP, TP),
            P(SP, TP),
            P(TP, SP),
        ),
        out_specs=P(SP, None),
        check_vma=False,
    )
```
